32 devices in a mesh: grp: 2 (over x), fs: 4 (over z), tp: 4 (over y, core).
Axes of the slice: x: 2, y: 2, z: 4, core: 2. Of those that a mesh axis runs over, the one named last changes fastest.
Arguments:
- tokens: bfloat16 [4096, 2048], P(('grp', 'fs')), parts along dimension 0, may hold values from -200 to 200
- norm_gain: float32 [2048], replicated, may hold values from 0.1 to 1.9
- value_weight: float32 [2048, 5632], P('fs', 'tp'), may hold values from -0.125 to 0.125
- gate_weight: float32 [2048, 5632], P('fs', 'tp'), may hold values from -0.125 to 0.125
- down_weight: float32 [2048, 5632], P('fs', 'tp'), may hold values from -0.078125 to 0.078125
- value_scale: float32 [5632], P('tp'), may hold values from 0.3 to 3
- gate_scale: float32 [5632], P('tp'), may hold values from 0.3 to 3
- down_scale: float32 [2048], replicated, may hold values from 0.3 to 3
- value_taps: float32 [3, 5632], P(None, 'tp'), may hold values from -3 to 3
- gate_taps: float32 [3, 5632], P(None, 'tp'), may hold values from -3 to 3
- value_bias: float32 [5632], P('tp'), may hold values from -3 to 3
- gate_bias: float32 [5632], P('tp'), may hold values from -3 to 3
Outputs:
- mixed: bfloat16 [4096, 2048], P(('grp', 'fs', 'tp')), parts along dimension 0
The draws below stay inside these ranges and needn't reach their ends.
There are 2 independent parts, one for each index of `grp`. The reference program is written for one: setup_inputs(seed, part) draws one part's arguments, and reference() takes and returns one part's arrays. A program takes and returns all parts, laid end to end along the dimension named above; an argument that names none is the same for every part. Nothing has to cross between parts.
All inputs are finite; a program needn't handle non-finite values.
Results may differ from the reference program's by a relative error of at most 0.024.
Values may be sent and summed in bfloat16 or wider, within the bound.
No kernel may reach another device: no remote copies, remote signals or barrier semaphores. Data moves between devices by JAX's collectives and lax.ppermute only.
A program may use at most 64 MiB of HBM per device.

```python
import math
import jax
import jax.numpy as jnp
from jax import lax

D = 2048
FF = 5632
TAPS = 3
ROWS = 512
TOKENS = 2048
N_FS = 4
N_TP = 4


def draw_tokens(key, part):
    key_base = jax.random.fold_in(key, 11)
    key_rows = jax.random.fold_in(key, 12)
    base = jnp.clip(jax.random.normal(key_base, (TOKENS, D), jnp.float32), -6.0, 6.0)
    spread = jax.random.uniform(key_rows, (TOKENS, 1), jnp.float32, 0.0, math.log(10.0))
    return (base * jnp.exp(spread)).astype(jnp.bfloat16)


def levels(rng, shape, split, smallest, high):
    def one(position, shards_of):
        steps = jax.random.uniform(jax.random.fold_in(jax.random.fold_in(rng, 6), position), (shards_of,), jnp.float32, smallest / len(split), high / len(split))
        return jnp.repeat(jnp.exp(steps), shape[position] // shards_of).reshape((-1,) + (1,) * (len(shape) - position - 1))

    level = one(*split[0])
    for cut in split[1:]:
        level = level * one(*cut)
    return level


def scatter_about(rng, extent, scale, reach, shards=(), kind=jnp.bfloat16):
    drawn = scale * jax.random.normal(rng, extent, jnp.float32)
    if shards:
        drawn = drawn * levels(rng, extent, shards, -0.22, 0.18)
    return jnp.clip(drawn, -reach, reach).astype(kind)


def setup_inputs(seed: int = 0, part: int = 0) -> dict:
    keys = jax.random.split(jax.random.key(seed), 13)
    part_keys = jax.random.split(jax.random.fold_in(keys[12], part), 13)
    tokens = draw_tokens(jax.random.fold_in(jax.random.fold_in(keys[12], part), 71), part)
    norm_gain = jnp.clip(1.0 + 0.18 * jax.random.normal(keys[1], (D,), jnp.float32), 0.1, 1.9)
    value_weight = scatter_about(keys[2], (D, FF), D ** -0.5, 0.125, ((0, 4), (1, 4)), jnp.float32)
    gate_weight = scatter_about(keys[3], (D, FF), D ** -0.5, 0.125, ((0, 4), (1, 4)), jnp.float32)
    down_weight = scatter_about(keys[4], (D, FF), FF ** -0.5, 0.078125, ((0, 4), (1, 4)), jnp.float32)
    value_scale = jnp.clip(jnp.exp(math.log(3.0) - 2.3025851 * jax.random.uniform(keys[5], (FF,), jnp.float32) ** levels(keys[5], (FF,), ((0, 4),), -0.2, 0.2)), 0.3, 3.0)
    gate_scale = jnp.clip(jnp.exp(math.log(3.0) - 2.3025851 * jax.random.uniform(keys[6], (FF,), jnp.float32) ** levels(keys[6], (FF,), ((0, 4),), -0.2, 0.2)), 0.3, 3.0)
    down_scale = jnp.clip(jnp.exp(jax.random.uniform(keys[7], (D,), jnp.float32, math.log(0.3), math.log(3.0))), 0.3, 3.0)
    value_taps = scatter_about(keys[8], (TAPS, FF), 0.577, 3.0, ((1, 4),), jnp.float32)
    gate_taps = scatter_about(keys[9], (TAPS, FF), 0.577, 3.0, ((1, 4),), jnp.float32)
    value_bias = scatter_about(keys[10], (FF,), 0.5, 3.0, ((0, 4),), jnp.float32)
    gate_bias = scatter_about(keys[11], (FF,), 0.5, 3.0, ((0, 4),), jnp.float32)
    return dict(tokens=tokens, norm_gain=norm_gain, value_weight=value_weight, gate_weight=gate_weight, down_weight=down_weight, value_scale=value_scale, gate_scale=gate_scale, down_scale=down_scale, value_taps=value_taps, gate_taps=gate_taps, value_bias=value_bias, gate_bias=gate_bias)


def causal_mix(field, taps, bias):
    back_one = jnp.pad(field, ((1, 0), (0, 0)))[:-1]
    back_two = jnp.pad(field, ((2, 0), (0, 0)))[:-2]
    return taps[0] * back_two + taps[1] * back_one + taps[2] * field + bias

def reference(tokens, norm_gain, value_weight, gate_weight, down_weight, value_scale, gate_scale, down_scale, value_taps, gate_taps, value_bias, gate_bias):
    value_cast = value_weight.astype(jnp.bfloat16)
    gate_cast = gate_weight.astype(jnp.bfloat16)
    down_cast = down_weight.astype(jnp.bfloat16)

    def one_sequence(rows):
        floated = rows.astype(jnp.float32)
        inverse = lax.rsqrt(lax.optimization_barrier(jnp.mean(floated * floated, axis=-1, keepdims=True)) + 1e-06)
        normed = (floated * inverse * norm_gain).astype(jnp.bfloat16)
        value_up = jnp.dot(normed, value_cast, preferred_element_type=jnp.float32) * value_scale
        gate_up = jnp.dot(normed, gate_cast, preferred_element_type=jnp.float32) * gate_scale
        value_mixed = causal_mix(value_up, value_taps, value_bias)
        gate_mixed = causal_mix(gate_up, gate_taps, gate_bias)
        return (jax.nn.silu(gate_mixed) * value_mixed).astype(jnp.bfloat16)
    hidden = lax.map(one_sequence, tokens.reshape(N_FS, ROWS, D)).reshape(N_FS * ROWS, FF)
    block = FF // N_TP

    def add_block(index, total):
        start = (index * block).astype(jnp.int32)
        left = lax.dynamic_slice_in_dim(hidden, start, block, 1)
        right = lax.dynamic_slice_in_dim(down_cast, start, block, 1)
        term = lax.dot_general(left, right, (((1,), (1,)), ((), ())), preferred_element_type=jnp.float32)
        return total + term.astype(jnp.bfloat16).astype(jnp.float32)
    total = lax.fori_loop(0, N_TP, add_block, jnp.zeros((N_FS * ROWS, D), jnp.float32))
    return (total * down_scale).astype(jnp.bfloat16)
```

```python
import jax
import jax.numpy as jnp
from jax import lax
from jax.sharding import PartitionSpec as P


def causal_mix(field, taps, bias):
    back_one = jnp.pad(field, ((0, 0), (1, 0), (0, 0)))[:, :-1]
    back_two = jnp.pad(field, ((0, 0), (2, 0), (0, 0)))[:, :-2]
    return taps[0] * back_two + taps[1] * back_one + taps[2] * field + bias


def build(groups, line, spread):
    place = lambda: lax.axis_index("fs")

    def relay(shards):
        right = [[shard] for shard in shards]
        left = [[shard] for shard in shards]
        for step in range(1, line):
            for r, l in zip(right, left):
                r.append(lax.ppermute(r[-1], "fs", [(i, i + 1) for i in range(step - 1, line - 1)]))
                l.append(lax.ppermute(l[-1], "fs", [(i, i - 1) for i in range(1, line - step + 1)]))
        return [
            [shard]
            + [jnp.where(place() >= k, r[k], l[line - k]) for k in range(1, line)]
            for shard, r, l in zip(shards, right, left)
        ]

    def add(a, b):
        return (a.astype(jnp.float32) + b.astype(jnp.float32)).astype(jnp.bfloat16)

    def reduce_block(block):
        pairs = spread // 2
        here = lax.axis_index("tp")
        core, chip = here % 2, here // 2
        features = block.shape[-1]
        block = block.reshape(groups, pairs, 2, -1, features)
        keep = lax.dynamic_index_in_dim(block, core, axis=2, keepdims=False)
        send = lax.dynamic_index_in_dim(block, 1 - core, axis=2, keepdims=False)
        block = add(keep, lax.ppermute(send, "tp", [(i, i ^ 1) for i in range(spread)]))
        total = block[0]
        for step in range(1, groups):
            total = add(
                total,
                lax.ppermute(
                    block[step], "grp", [((i + step) % groups, i) for i in range(groups)]
                ),
            )
        out = lax.dynamic_index_in_dim(total, chip, axis=0, keepdims=False).astype(jnp.float32)
        for step in range(1, pairs):
            send = lax.dynamic_index_in_dim(total, (chip + step) % pairs, axis=0, keepdims=False)
            got = lax.ppermute(
                send, "tp", [(i, (i + 2 * step) % spread) for i in range(spread)]
            )
            out = out + got.astype(jnp.float32)
        return out

    def local(
        tokens,
        norm_gain,
        value_weight,
        gate_weight,
        down_weight,
        value_scale,
        gate_scale,
        down_scale,
        value_taps,
        gate_taps,
        value_bias,
        gate_bias,
    ):
        units = value_weight.shape[1] // groups
        first = lax.axis_index("grp") * units

        def mine(array):
            return lax.dynamic_slice_in_dim(array, first, units, axis=array.ndim - 1)

        value_cast = mine(value_weight).astype(jnp.bfloat16)
        gate_cast = mine(gate_weight).astype(jnp.bfloat16)
        down_cast = mine(down_weight).astype(jnp.bfloat16)
        values, gates = relay([value_cast, gate_cast])
        (downs,) = relay([down_cast])
        floated = tokens.astype(jnp.float32)
        inverse = lax.rsqrt(jnp.mean(floated * floated, axis=-1, keepdims=True) + 1e-06)
        normed = (floated * inverse * norm_gain).astype(jnp.bfloat16)
        rows = normed.shape[0]
        held = [normed]
        for step in range(1, groups):
            held.append(
                lax.ppermute(normed, "grp", [(i, (i + step) % groups) for i in range(groups)])
            )
        both = jnp.concatenate(held, axis=0)
        width = value_cast.shape[0]
        value_up = gate_up = None
        for k in range(line):
            part = lax.dynamic_slice_in_dim(both, ((place() - k) % line) * width, width, axis=1)
            v = jnp.dot(part, values[k], preferred_element_type=jnp.float32)
            g = jnp.dot(part, gates[k], preferred_element_type=jnp.float32)
            value_up = v if k == 0 else value_up + v
            gate_up = g if k == 0 else gate_up + g
        value_up = (value_up * mine(value_scale)).reshape(groups, rows, units)
        gate_up = (gate_up * mine(gate_scale)).reshape(groups, rows, units)
        value_mixed = causal_mix(value_up, mine(value_taps), mine(value_bias))
        gate_mixed = causal_mix(gate_up, mine(gate_taps), mine(gate_bias))
        hidden = (jax.nn.silu(gate_mixed) * value_mixed).astype(jnp.bfloat16)
        hidden = hidden.reshape(groups * rows, units)
        blocks = []
        for k in range(line):
            block = lax.dot_general(
                hidden, downs[k], (((1,), (1,)), ((), ())), preferred_element_type=jnp.float32
            ).astype(jnp.bfloat16)
            blocks.append(reduce_block(block))
        ordered = jnp.stack(blocks[::-1])
        ordered = jnp.roll(ordered, place() + 1, axis=0)
        total = ordered.transpose(1, 0, 2).reshape(ordered.shape[1], -1)
        return (total * down_scale).astype(jnp.bfloat16)

    return local


def solution(mesh):
    return jax.shard_map(
        build(mesh.shape["grp"], mesh.shape["fs"], mesh.shape["tp"]),
        mesh=mesh,
        in_specs=(
            P(("grp", "fs"), None),
            P(),
            P("fs", "tp"),
            P("fs", "tp"),
            P("fs", "tp"),
            P("tp"),
            P("tp"),
            P(),
            P(None, "tp"),
            P(None, "tp"),
            P("tp"),
            P("tp"),
        ),
        out_specs=P(("grp", "fs", "tp"), None),
        check_vma=False,
    )
```
